1024 devices in a mesh: ep: 32 (over z, core), tp: 32 (over y, x).
Axes of the slice: x: 4, y: 8, z: 16, core: 2. Of those that a mesh axis runs over, the one named last changes fastest.
Arguments:
- tokens: bfloat16 [512, 4096], P('ep', 'tp'), may hold values from -40 to 40
- routes: int32 [512, 4], P('ep'), may hold values from 0 to 63, all different within a row; in each aligned block of 16 rows (0 to 15, 16 to 31, ...) at most 2 rows name the same one
- gates: float32 [512, 4], P('ep'), may hold values from 0.1 to 1
- pre_gain: bfloat16 [4096], P('tp'), may hold values from 0.099609375 to 1.8984375
- expert_gate: bfloat16 [64, 4096, 1024], P('ep', 'tp'), may hold values from -0.09375 to 0.09375
- expert_up: bfloat16 [64, 4096, 1024], P('ep', 'tp'), may hold values from -0.09375 to 0.09375
- expert_down: bfloat16 [64, 1024, 4096], P('ep', None, 'tp'), may hold values from -0.125 to 0.125
- shared_gate: bfloat16 [4096, 1024], P('tp'), may hold values from -0.09375 to 0.09375
- shared_up: bfloat16 [4096, 1024], P('tp'), may hold values from -0.09375 to 0.09375
- shared_down: bfloat16 [1024, 4096], P(None, 'tp'), may hold values from -0.125 to 0.125
- out_gain: bfloat16 [4096], P('tp'), may hold values from 0.099609375 to 1.8984375
Outputs:
- mixed: bfloat16 [512, 4096], P('ep', 'tp')
The draws below stay inside these ranges and needn't reach their ends.
Inputs may be any that keep to these rules, and one draw needn't show every extreme that they name: `routes`: each row names 4 different experts, and expert e is held by index e // 2 of ep. Among the 16 rows of one index of ep no expert is named by more than 2 rows, and in every draw some expert is named by exactly 2 rows of some index.
All inputs are finite; a program needn't handle non-finite values.
Results may differ from the reference program's by a relative error of at most 0.012.
Values may be sent and summed in bfloat16 or wider, within the bound.
No kernel may reach another device: no remote copies, remote signals or barrier semaphores. Data moves between devices by JAX's collectives and lax.ppermute only.
A program may use at most 32 MiB of HBM per device.

```python
import math
import jax
import jax.numpy as jnp
import numpy as np
from jax import lax

D = 4096
FE = 1024
FS = 1024
TOP = 4
TOK_DEV = 16
EXPERTS = 64
CAP = 2
TOKENS = 512
N_EP = 32


def scaled_columns(key, shape, fan_in):
    first = jax.random.fold_in(key, 0)
    position = jnp.arange(shape[-1], dtype=jnp.float32) / shape[-1]
    base = jnp.clip(jax.random.normal(first, shape, jnp.float32), -4.0, 4.0)
    column = 10.0 ** (position - 1.0)
    return base * column * fan_in ** (-0.5)


def draw_expert_down(key, part):
    return scaled_columns(jax.random.fold_in(key, 11), (EXPERTS, FE, D), FE).astype(jnp.bfloat16)


def draw_shared_down(key, part):
    return scaled_columns(jax.random.fold_in(key, 12), (FS, D), FS).astype(jnp.bfloat16)


def draw_tokens(key, part):
    first, second = jax.random.split(jax.random.fold_in(key, 13), 2)
    position = jnp.arange(D, dtype=jnp.float32) / D
    row_scale = 10.0 ** jax.random.uniform(second, (TOKENS, 1), jnp.float32)
    base = jnp.clip(jax.random.normal(first, (TOKENS, D), jnp.float32), -4.0, 4.0)
    column = 10.0 ** position
    return (base * column * row_scale / 10.0).astype(jnp.bfloat16)


def shard_levels(own_key, shape, cuts, low, high):
    def one(dim, parts):
        heights = jax.random.uniform(jax.random.fold_in(jax.random.fold_in(own_key, 6), dim), (parts,), jnp.float32, low / len(cuts), high / len(cuts))
        return jnp.repeat(jnp.exp(heights), shape[dim] // parts).reshape((-1,) + (1,) * (len(shape) - dim - 1))

    level = one(*cuts[0])
    for cut in cuts[1:]:
        level = level * one(*cut)
    return level


def assign_block(key, own, number, rows, count, top, limit, slope):
    order = jax.random.permutation(key, count)
    crowded, ordinary = load_shares(count, rows * top, limit, slope, True), load_shares(count, rows * top, limit, slope, False)
    places = jnp.arange(count)

    def named(lengths, turn):
        used = int((lengths > 0).sum())
        fixed = max(1, used // 4)
        shifted = fixed + (places - fixed + turn * (used - fixed)) % max(1, count - fixed)
        return jnp.zeros((count,), jnp.int32).at[order[jnp.where(places < fixed, places, shifted)]].set(jnp.asarray(lengths, jnp.int32))

    lengths = jnp.where(number % 4 == 0, named(crowded, number // 4), named(ordinary, number - number // 4 - 1))
    mixed = jax.random.permutation(jax.random.fold_in(own, 3), count)
    giver, taker = mixed[0:count // 2 * 2:2], mixed[1:count // 2 * 2:2]
    margin = jnp.minimum(lengths[giver] - 1, limit - lengths[taker]) // 2
    margin = jnp.where((giver == order[0]) | (taker == order[0]) | (lengths[taker] == 0), 0, jnp.maximum(margin, 0))
    shifted = jax.random.randint(jax.random.fold_in(own, 4), (count // 2,), 0, 1 << 20) % (margin + 1)
    lengths = lengths.at[giver].add(-shifted).at[taker].add(shifted)
    members = jnp.searchsorted(jnp.cumsum(lengths), jnp.arange(rows * top), side="right").astype(jnp.int32)
    table = members.reshape(top, rows).T
    table = table[jax.random.permutation(jax.random.fold_in(own, 1), rows)]
    turn = jax.random.randint(jax.random.fold_in(own, 2), (rows, 1), 0, top)
    return jnp.take_along_axis(table, (jnp.arange(top)[None, :] + turn) % top, axis=1)


def load_shares(number_of, total, most, lean, full):
    loads = [(1 << 20) // math.isqrt(standing ** lean) + 1 for standing in range(1, number_of + 1)]
    largest = most if full else min(most, max(-(-total // number_of), total * loads[0] // sum(loads)))
    least = 1 if total - largest >= number_of - 1 else 0
    given, rest = [largest] + [least] * (number_of - 1), total - largest - least * (number_of - 1)
    while rest > 0:
        movable = [i for i in range(1, number_of) if given[i] < largest] or [i for i in range(1, number_of) if given[i] < most]
        pool, remaining = sum([loads[i] for i in movable]), rest
        for i in movable:
            extra = min(most - given[i], max(1, remaining * loads[i] // pool), rest)
            given[i] = given[i] + extra
            rest = rest - extra
    return np.array(given)


def normal_values(own_key, shape, width, most, pieces=(), held_as=jnp.bfloat16):
    array = jax.random.normal(own_key, shape, jnp.float32) * width
    if len(pieces) > 0:
        array = shard_levels(own_key, shape, pieces, -0.22, 0.18) * array
    return jnp.clip(array, min=-most, max=most).astype(held_as)


def setup_inputs(seed: int = 0) -> dict:
    key_list = jax.random.split(jax.random.key(seed), 12)
    tokens = draw_tokens(jax.random.fold_in(key_list[11], 71), 0)
    routes_keys = jax.random.split(jax.random.fold_in(key_list[1], 1), TOKENS // TOK_DEV)
    routes_turns = jax.random.permutation(jax.random.fold_in(key_list[1], 3), TOKENS // TOK_DEV)
    routes = jax.vmap(lambda own, number: assign_block(jax.random.fold_in(key_list[1], 2), own, number, TOK_DEV, EXPERTS, TOP, CAP, 2))(routes_keys, routes_turns).reshape((TOKENS, TOP))
    gates = jnp.clip(jnp.exp(math.log(1.0) - 2.3025851 * jax.random.uniform(key_list[2], (TOKENS, TOP), jnp.float32) ** shard_levels(key_list[2], (TOKENS, TOP), ((0, 32),), -0.2, 0.2)), 0.1, 1.0)
    pre_gain = jnp.clip(1.0 + 0.18 * jax.random.normal(key_list[3], (D,), jnp.float32), 0.099609375, 1.8984375).astype(jnp.bfloat16)
    expert_gate = normal_values(key_list[4], (EXPERTS, D, FE), D ** -0.5, 0.09375, ((0, 32), (1, 32)))
    expert_up = normal_values(key_list[5], (EXPERTS, D, FE), D ** -0.5, 0.09375, ((0, 32), (1, 32)))
    expert_down = draw_expert_down(jax.random.fold_in(key_list[11], 71), 0)
    shared_gate = normal_values(key_list[7], (D, FS), D ** -0.5, 0.09375, ((0, 32),))
    shared_up = normal_values(key_list[8], (D, FS), D ** -0.5, 0.09375, ((0, 32),))
    shared_down = draw_shared_down(jax.random.fold_in(key_list[11], 71), 0)
    out_gain = jnp.clip(1.0 + 0.18 * jax.random.normal(key_list[10], (D,), jnp.float32), 0.099609375, 1.8984375).astype(jnp.bfloat16)
    return dict(tokens=tokens, routes=routes, gates=gates, pre_gain=pre_gain, expert_gate=expert_gate, expert_up=expert_up, expert_down=expert_down, shared_gate=shared_gate, shared_up=shared_up, shared_down=shared_down, out_gain=out_gain)


def normalize(values, gain):
    as_float = values.astype(jnp.float32)
    scale = lax.rsqrt(lax.optimization_barrier(jnp.mean(as_float * as_float, axis=-1, keepdims=True)) + 1e-06)
    return as_float * scale * gain.astype(jnp.float32)

def reference(tokens, routes, gates, pre_gain, expert_gate, expert_up, expert_down, shared_gate, shared_up, shared_down, out_gain):
    normed = normalize(tokens, pre_gain).astype(jnp.bfloat16)
    labels = jnp.arange(EXPERTS, dtype=jnp.int32)
    picked = routes[:, :, None] == labels[None, None, :]
    onehot = lax.optimization_barrier(jnp.sum(picked.astype(jnp.int32), axis=1))
    dense_gate = lax.optimization_barrier(jnp.sum(jnp.where(picked, gates[:, :, None], jnp.zeros((), jnp.float32)), axis=1))
    blocked = onehot.reshape(N_EP, TOK_DEV, EXPERTS)
    slot_index = (jnp.cumsum(blocked, axis=1) - blocked).reshape(TOKENS, EXPERTS).astype(jnp.int32)
    block_of = jnp.arange(TOKENS, dtype=jnp.int32) // TOK_DEV
    target_row = jnp.where(onehot > 0, block_of[:, None] * CAP + slot_index, -1).astype(jnp.int32)
    row_index = jnp.arange(N_EP * CAP, dtype=jnp.int32)

    def per_expert(accumulated, expert_index):
        select = row_index[:, None] == target_row[:, expert_index][None, :]
        buffer = jnp.dot(select.astype(jnp.bfloat16), normed, preferred_element_type=jnp.float32).astype(jnp.bfloat16)
        gate_act = jnp.dot(buffer, expert_gate[expert_index], preferred_element_type=jnp.float32)
        up_act = jnp.dot(buffer, expert_up[expert_index], preferred_element_type=jnp.float32)
        hidden = (jax.nn.silu(gate_act) * up_act).astype(jnp.bfloat16)
        result = jnp.dot(hidden, expert_down[expert_index], preferred_element_type=jnp.float32).astype(jnp.bfloat16)
        weight = jnp.where(select, dense_gate[:, expert_index][None, :], jnp.zeros((), jnp.float32))
        accumulated = accumulated + jnp.dot(weight.T, result.astype(jnp.float32), precision=lax.Precision.HIGHEST)
        return (accumulated, None)
    routed, _ = lax.scan(per_expert, jnp.zeros((TOKENS, D), jnp.float32), jnp.arange(EXPERTS, dtype=jnp.int32))
    shared_gate_act = jnp.dot(normed, shared_gate, preferred_element_type=jnp.float32)
    shared_up_act = jnp.dot(normed, shared_up, preferred_element_type=jnp.float32)
    shared_hidden = (jax.nn.silu(shared_gate_act) * shared_up_act).astype(jnp.bfloat16)
    shared_out = jnp.dot(shared_hidden, shared_down, preferred_element_type=jnp.float32)
    combined = routed + shared_out
    return normalize(combined, out_gain).astype(jnp.bfloat16)
```

```python
import jax
import jax.numpy as jnp
from jax import lax
from jax.experimental import pallas as pl
from jax.experimental.pallas import tpu as pltpu
from jax.sharding import PartitionSpec as P

D = 4096
EPS = 1e-06
PEERS = 32
LANES = 128
ROWS = 128
GROUPS = 4
BLOCK = 80
HID = 40
F32 = jnp.float32
BF16 = jnp.bfloat16
I32 = jnp.int32


def iota(shape, dim):
    return lax.broadcasted_iota(I32, shape, dim)


def dot(a, b):
    return jnp.dot(a, b, preferred_element_type=F32)


def slot_choice(routes_t):
    tok = routes_t.shape[1]
    slot = iota((ROWS, tok), 0)
    expert = slot >> 1
    named = jnp.zeros((ROWS, tok), F32)
    for k in range(4):
        named = named + jnp.where(routes_t[k : k + 1, :] == expert, 1.0, 0.0)
    earlier = jnp.where(iota((tok, tok), 0) < iota((tok, tok), 1), 1.0, 0.0)
    before = dot(named.astype(BF16), earlier.astype(BF16))
    place = (slot & 1).astype(F32)
    return jnp.where((named > 0.5) & (before == place), 1.0, 0.0)


def dispatch_kernel(tokens_ref, routes_ref, out_ref):
    choice = slot_choice(routes_ref[...])
    out_ref[...] = dot(choice.astype(BF16), tokens_ref[...]).astype(BF16)


def row_of(col, lanes_from):
    n = col.shape[0]
    hit = iota((n, LANES), 1) == iota((n, LANES), 0) + lanes_from
    return jnp.sum(jnp.where(hit, col, 0.0), axis=0, keepdims=True)


def col_of(row, n, lanes_from):
    hit = iota((n, LANES), 1) == iota((n, LANES), 0) + lanes_from
    return jnp.sum(jnp.where(hit, row, 0.0), axis=1, keepdims=True)


def project_kernel(recv_ref, tokens_ref, gain_ref, wg_ref, wu_ref, sg_ref, su_ref, out_ref):
    gain = gain_ref[...].astype(F32)
    to_row = iota((ROWS, ROWS), 0)
    from_row = ((to_row & 31) << 2) + (to_row >> 5)
    swap = jnp.where(iota((ROWS, ROWS), 1) == from_row, 1.0, 0.0).astype(BF16)
    rows = dot(swap, recv_ref[...])
    row_sq = jnp.sum(rows * rows, axis=1, keepdims=True)
    scaled = (rows * gain).astype(BF16)
    tr = iota((32, 16), 0)
    take = jnp.where(iota((32, 16), 1) == ((tr >> 3) << 2) + (tr & 3), 1.0, 0.0).astype(BF16)
    toks = dot(take, tokens_ref[...])
    tok_sq = jnp.sum(toks * toks, axis=1, keepdims=True)
    toks_scaled = (toks * gain).astype(BF16)
    shared_g = dot(toks_scaled, sg_ref[...])
    shared_u = dot(toks_scaled, su_ref[...])
    shared = jnp.where((iota((32, 1024), 0) & 7) < 4, shared_g, shared_u)
    sub = iota((8, LANES), 0)
    for e in range(2):
        x = scaled[64 * e : 64 * e + 64]
        g = dot(x, wg_ref[e]).astype(BF16)
        u = dot(x, wu_ref[e]).astype(BF16)
        for c in range(2):
            r = 2 * e + c
            sq = row_of(row_sq[32 * r : 32 * r + 32], 0) + row_of(tok_sq[8 * r : 8 * r + 8], 64)
            hi = sq.astype(BF16).astype(F32)
            lo = sq - hi
            sq8 = jnp.where(sub == 0, hi, jnp.where(sub == 1, lo, 0.0))
            for l in range(8):
                p = 8 * r + l
                cols = slice(128 * l, 128 * l + 128)
                out_ref[p, 0:32, :] = g[32 * c : 32 * c + 32, cols]
                out_ref[p, 32:64, :] = u[32 * c : 32 * c + 32, cols]
                tail = jnp.concatenate([shared[8 * r : 8 * r + 8, cols], sq8], axis=0)
                out_ref[p, 64:80, :] = tail.astype(BF16)


def silu(v):
    return v / (1.0 + jnp.exp(-v))


def hidden_kernel(recv_ref, out_ref):
    total = jnp.sum(recv_ref[...].astype(F32), axis=0)
    sq = total[72:73] + total[73:74]
    row_scale = lax.rsqrt(col_of(sq, 32, 0) / D + EPS)
    hid = silu(total[0:32] * row_scale) * (total[32:64] * row_scale)
    tok_scale = lax.rsqrt(col_of(sq, 8, 64) / D + EPS)
    both = total[64:72] * tok_scale
    up = pltpu.roll(both, 4, 0)
    shared = jnp.where(iota((8, LANES), 0) < 4, silu(both) * up, 0.0)
    piece = jnp.concatenate([hid, shared], axis=0).astype(BF16)
    out_ref[...] = jnp.broadcast_to(piece[None], out_ref.shape)


def down_kernel(recv_ref, wd_ref, out_ref):
    parts = []
    for e in range(2):
        lhs = jnp.concatenate(
            [
                jnp.concatenate([recv_ref[8 * (2 * e + c) + l, 0:32, :] for l in range(8)], axis=1)
                for c in range(2)
            ],
            axis=0,
        )
        parts.append(dot(lhs, wd_ref[e]).astype(BF16))
    rows = jnp.concatenate(parts, axis=0)
    to_row = iota((ROWS, ROWS), 0)
    from_row = ((to_row & 3) << 5) + (to_row >> 2)
    swap = jnp.where(iota((ROWS, ROWS), 1) == from_row, 1.0, 0.0).astype(BF16)
    out_ref[...] = dot(swap, rows).astype(BF16)


def shared_kernel(recv_ref, sd_ref, routes_ref, gates_ref, shared_ref, weight_ref):
    lhs = jnp.concatenate(
        [
            jnp.concatenate([recv_ref[8 * r + l, 32:40, :] for l in range(8)], axis=1)
            for r in range(4)
        ],
        axis=0,
    )
    full = dot(lhs, sd_ref[...])
    shared_ref[...] = jnp.concatenate([full[8 * r : 8 * r + 4] for r in range(4)], axis=0)
    routes_t = routes_ref[...]
    gates_t = gates_ref[...]
    choice = slot_choice(routes_t)
    expert = iota(choice.shape, 0) >> 1
    gate = jnp.zeros(choice.shape, F32)
    for k in range(4):
        gate = gate + jnp.where(routes_t[k : k + 1, :] == expert, gates_t[k : k + 1, :], 0.0)
    weight_ref[...] = jnp.transpose(choice * gate)


def combine_kernel(recv_ref, weight_ref, shared_ref, out_ref, sq_ref):
    routed = jnp.dot(
        weight_ref[...],
        recv_ref[...].astype(F32),
        precision=lax.Precision.HIGHEST,
        preferred_element_type=F32,
    )
    combined = routed + shared_ref[...]
    out_ref[...] = combined
    sq = row_of(jnp.sum(combined * combined, axis=1, keepdims=True), 0)
    sq_ref[...] = jnp.broadcast_to(sq[None], sq_ref.shape)


def final_kernel(sq_ref, combined_ref, gain_ref, out_ref):
    sq = jnp.sum(sq_ref[...], axis=0)
    scale = lax.rsqrt(col_of(sq, 16, 0) / D + EPS)
    out_ref[...] = (combined_ref[...] * scale * gain_ref[...].astype(F32)).astype(BF16)


def call(kernel, out, *args):
    return pl.pallas_call(kernel, out_shape=out)(*args)


def shape(dims, dtype):
    return jax.ShapeDtypeStruct(dims, dtype)


def swapped(x, axis):
    return lax.all_to_all(x, axis, 0, 0, tiled=True)


def on_device(
    tokens,
    routes,
    gates,
    pre_gain,
    expert_gate,
    expert_up,
    expert_down,
    shared_gate,
    shared_up,
    shared_down,
    out_gain,
):
    routes_t = routes.T
    gates_t = gates.T
    outgoing = call(dispatch_kernel, shape((ROWS, LANES), BF16), tokens, routes_t)
    received = swapped(outgoing.reshape(PEERS, GROUPS, LANES), "ep").reshape(ROWS, LANES)
    partial = call(
        project_kernel,
        shape((PEERS, BLOCK, LANES), BF16),
        received,
        tokens,
        pre_gain.reshape(1, LANES),
        expert_gate,
        expert_up,
        shared_gate,
        shared_up,
    )
    summands = swapped(partial, "tp")
    piece = call(hidden_kernel, shape((PEERS, HID, LANES), BF16), summands)
    hidden = swapped(piece, "tp")
    results = call(down_kernel, shape((ROWS, LANES), BF16), hidden, expert_down)
    returned = swapped(results.reshape(PEERS, GROUPS, LANES), "ep").reshape(ROWS, LANES)
    shared_out, weight = call(
        shared_kernel,
        (shape((16, LANES), F32), shape((16, ROWS), F32)),
        hidden,
        shared_down,
        routes_t,
        gates_t,
    )
    combined, squares = call(
        combine_kernel,
        (shape((16, LANES), F32), shape((PEERS, 1, LANES), F32)),
        returned,
        weight,
        shared_out,
    )
    squares = swapped(squares, "tp")
    return call(
        final_kernel,
        shape((16, LANES), BF16),
        squares,
        combined,
        out_gain.reshape(1, LANES),
    )


def solution(mesh):
    in_specs = (
        P("ep", "tp"),
        P("ep", None),
        P("ep", None),
        P("tp"),
        P("ep", "tp", None),
        P("ep", "tp", None),
        P("ep", None, "tp"),
        P("tp", None),
        P("tp", None),
        P(None, "tp"),
        P("tp"),
    )
    return jax.shard_map(
        on_device, mesh=mesh, in_specs=in_specs, out_specs=P("ep", "tp"), check_vma=False
    )
```

```python
import jax
import jax.numpy as jnp
from jax import lax
from jax.experimental import pallas as pl
from jax.experimental.pallas import tpu as pltpu
from jax.sharding import PartitionSpec as P

D = 4096
EPS = 1e-06
PEERS = 32
LANES = 128
ROWS = 128
GROUPS = 4
BLOCK = 80
HID = 40
F32 = jnp.float32
BF16 = jnp.bfloat16
I32 = jnp.int32


def iota(shape, dim):
    return lax.broadcasted_iota(I32, shape, dim)


def dot(a, b):
    return jnp.dot(a, b, preferred_element_type=F32)


def slot_choice(routes_t):
    tok = routes_t.shape[1]
    slot = iota((ROWS, tok), 0)
    expert = slot >> 1
    named = jnp.zeros((ROWS, tok), F32)
    for k in range(4):
        named = named + jnp.where(routes_t[k : k + 1, :] == expert, 1.0, 0.0)
    earlier = jnp.where(iota((tok, tok), 0) < iota((tok, tok), 1), 1.0, 0.0)
    before = dot(named.astype(BF16), earlier.astype(BF16))
    place = (slot & 1).astype(F32)
    return jnp.where((named > 0.5) & (before == place), 1.0, 0.0)


def loads(pairs, sems):
    copies = [pltpu.make_async_copy(src, dst, sems.at[i]) for i, (src, dst) in enumerate(pairs)]
    for c in copies:
        c.start()
    return copies


def dispatch_kernel(
    tokens_in, routes_in, gain_in, wg_in, wu_in, sg_in, su_in,
    out_ref, tokens_ref, routes_ref, gain_ref, wg_ref, wu_ref, sg_ref, su_ref, sems,
):
    copies = loads(
        (
            (routes_in, routes_ref),
            (tokens_in, tokens_ref),
            (gain_in, gain_ref),
            (wg_in, wg_ref),
            (wu_in, wu_ref),
            (sg_in, sg_ref),
            (su_in, su_ref),
        ),
        sems,
    )
    copies[0].wait()
    choice = slot_choice(routes_ref[...])
    copies[1].wait()
    out_ref[...] = dot(choice.astype(BF16), tokens_ref[...]).astype(BF16)
    for c in copies[2:]:
        c.wait()


def row_of(col, lanes_from):
    n = col.shape[0]
    hit = iota((n, LANES), 1) == iota((n, LANES), 0) + lanes_from
    return jnp.sum(jnp.where(hit, col, 0.0), axis=0, keepdims=True)


def col_of(row, n, lanes_from):
    hit = iota((n, LANES), 1) == iota((n, LANES), 0) + lanes_from
    return jnp.sum(jnp.where(hit, row, 0.0), axis=1, keepdims=True)


def project_kernel(
    recv_ref, tokens_ref, gain_ref, wg_ref, wu_ref, sg_ref, su_ref, wd_in, sd_in, gates_in, last_in,
    out_ref, wd_ref, sd_ref, gates_ref, last_ref, sems,
):
    copies = loads(
        ((wd_in, wd_ref), (sd_in, sd_ref), (gates_in, gates_ref), (last_in, last_ref)), sems
    )
    gain = gain_ref[...].astype(F32)
    to_row = iota((ROWS, ROWS), 0)
    from_row = ((to_row & 31) << 2) + (to_row >> 5)
    swap = jnp.where(iota((ROWS, ROWS), 1) == from_row, 1.0, 0.0).astype(BF16)
    rows = dot(swap, recv_ref[...])
    row_sq = jnp.sum(rows * rows, axis=1, keepdims=True)
    scaled = (rows * gain).astype(BF16)
    tr = iota((32, 16), 0)
    take = jnp.where(iota((32, 16), 1) == ((tr >> 3) << 2) + (tr & 3), 1.0, 0.0).astype(BF16)
    toks = dot(take, tokens_ref[...])
    tok_sq = jnp.sum(toks * toks, axis=1, keepdims=True)
    toks_scaled = (toks * gain).astype(BF16)
    shared_g = dot(toks_scaled, sg_ref[...])
    shared_u = dot(toks_scaled, su_ref[...])
    shared = jnp.where((iota((32, 1024), 0) & 7) < 4, shared_g, shared_u)
    sub = iota((8, LANES), 0)
    for e in range(2):
        x = scaled[64 * e : 64 * e + 64]
        g = dot(x, wg_ref[e]).astype(BF16)
        u = dot(x, wu_ref[e]).astype(BF16)
        for c in range(2):
            r = 2 * e + c
            sq = row_of(row_sq[32 * r : 32 * r + 32], 0) + row_of(tok_sq[8 * r : 8 * r + 8], 64)
            hi = sq.astype(BF16).astype(F32)
            lo = sq - hi
            sq8 = jnp.where(sub == 0, hi, jnp.where(sub == 1, lo, 0.0))
            for l in range(8):
                p = 8 * r + l
                cols = slice(128 * l, 128 * l + 128)
                out_ref[p, 0:32, :] = g[32 * c : 32 * c + 32, cols]
                out_ref[p, 32:64, :] = u[32 * c : 32 * c + 32, cols]
                tail = jnp.concatenate([shared[8 * r : 8 * r + 8, cols], sq8], axis=0)
                out_ref[p, 64:80, :] = tail.astype(BF16)
    for copy in copies:
        copy.wait()


def silu(v):
    return v / (1.0 + jnp.exp(-v))


def hidden_kernel(recv_ref, out_ref):
    total = jnp.sum(recv_ref[...].astype(F32), axis=0)
    sq = total[72:73] + total[73:74]
    row_scale = lax.rsqrt(col_of(sq, 32, 0) / D + EPS)
    hid = silu(total[0:32] * row_scale) * (total[32:64] * row_scale)
    tok_scale = lax.rsqrt(col_of(sq, 8, 64) / D + EPS)
    both = total[64:72] * tok_scale
    up = pltpu.roll(both, 4, 0)
    shared = jnp.where(iota((8, LANES), 0) < 4, silu(both) * up, 0.0)
    piece = jnp.concatenate([hid, shared], axis=0).astype(BF16)
    out_ref[...] = jnp.broadcast_to(piece[None], out_ref.shape)


def down_kernel(
    recv_ref, wd_ref, sd_ref, routes_ref, gates_ref, out_ref, shared_ref, weight_ref
):
    parts = []
    for e in range(2):
        lhs = jnp.concatenate(
            [
                jnp.concatenate([recv_ref[8 * (2 * e + c) + l, 0:32, :] for l in range(8)], axis=1)
                for c in range(2)
            ],
            axis=0,
        )
        parts.append(dot(lhs, wd_ref[e]).astype(BF16))
    rows = jnp.concatenate(parts, axis=0)
    to_row = iota((ROWS, ROWS), 0)
    from_row = ((to_row & 3) << 5) + (to_row >> 2)
    swap = jnp.where(iota((ROWS, ROWS), 1) == from_row, 1.0, 0.0).astype(BF16)
    out_ref[...] = dot(swap, rows).astype(BF16)
    lhs = jnp.concatenate(
        [
            jnp.concatenate([recv_ref[8 * r + l, 32:40, :] for l in range(8)], axis=1)
            for r in range(4)
        ],
        axis=0,
    )
    full = dot(lhs, sd_ref[...])
    shared_ref[...] = jnp.concatenate([full[8 * r : 8 * r + 4] for r in range(4)], axis=0)
    routes_t = routes_ref[...]
    gates_t = gates_ref[...]
    choice = slot_choice(routes_t)
    expert = iota(choice.shape, 0) >> 1
    gate = jnp.zeros(choice.shape, F32)
    for k in range(4):
        gate = gate + jnp.where(routes_t[k : k + 1, :] == expert, gates_t[k : k + 1, :], 0.0)
    weight_ref[...] = jnp.transpose(choice * gate)


def combine_kernel(recv_ref, weight_ref, shared_ref, out_ref, sq_ref):
    routed = jnp.dot(
        weight_ref[...],
        recv_ref[...].astype(F32),
        precision=lax.Precision.HIGHEST,
        preferred_element_type=F32,
    )
    combined = routed + shared_ref[...]
    out_ref[...] = combined
    sq = row_of(jnp.sum(combined * combined, axis=1, keepdims=True), 0)
    sq_ref[...] = jnp.broadcast_to(sq[None], sq_ref.shape)


def final_kernel(sq_ref, combined_ref, gain_ref, out_ref):
    sq = jnp.sum(sq_ref[...], axis=0)
    scale = lax.rsqrt(col_of(sq, 16, 0) / D + EPS)
    out_ref[...] = (combined_ref[...] * scale * gain_ref[...].astype(F32)).astype(BF16)


def call(kernel, out, fast, slow=()):
    return pl.pallas_call(
        kernel,
        out_shape=out,
        in_specs=[pl.BlockSpec(memory_space=pltpu.VMEM)] * len(fast)
        + [pl.BlockSpec(memory_space=pltpu.HBM)] * len(slow),
        scratch_shapes=[pltpu.SemaphoreType.DMA((len(slow),))] if slow else [],
        compiler_params=pltpu.CompilerParams(vmem_limit_bytes=16 << 20),
    )(*[pltpu.with_memory_space_constraint(a, pltpu.VMEM) for a in fast], *[pltpu.with_memory_space_constraint(a, pltpu.HBM) for a in slow])


def fast(dims, dtype):
    return pltpu.VMEM(dims, dtype)


def like(a):
    return pltpu.VMEM(a.shape, a.dtype)


def swapped(x, axis):
    return lax.all_to_all(x, axis, 0, 0, tiled=True)


def on_device(
    tokens,
    routes,
    gates,
    pre_gain,
    expert_gate,
    expert_up,
    expert_down,
    shared_gate,
    shared_up,
    shared_down,
    out_gain,
):
    first = (
        tokens,
        routes.T,
        pre_gain.reshape(1, LANES),
        expert_gate,
        expert_up,
        shared_gate,
        shared_up,
    )
    outgoing, tokens, routes, gain, *weights = call(
        dispatch_kernel, (fast((ROWS, LANES), BF16), *[like(a) for a in first]), (), first
    )
    received = swapped(outgoing.reshape(PEERS, GROUPS, LANES), "ep").reshape(ROWS, LANES)
    later = (expert_down, shared_down, gates.T, out_gain.reshape(1, LANES))
    partial, expert_down, shared_down, gates, out_gain = call(
        project_kernel,
        (fast((PEERS, BLOCK, LANES), BF16), *[like(a) for a in later]),
        (received, tokens, gain, *weights),
        later,
    )
    summands = swapped(partial, "tp")
    piece = call(hidden_kernel, fast((PEERS, HID, LANES), BF16), (summands,))
    hidden = swapped(piece, "tp")
    results, shared_out, weight = call(
        down_kernel,
        (fast((ROWS, LANES), BF16), fast((16, LANES), F32), fast((16, ROWS), F32)),
        (hidden, expert_down, shared_down, routes, gates),
    )
    returned = swapped(results.reshape(PEERS, GROUPS, LANES), "ep").reshape(ROWS, LANES)
    combined, squares = call(
        combine_kernel,
        (fast((16, LANES), F32), fast((PEERS, 1, LANES), F32)),
        (returned, weight, shared_out),
    )
    squares = swapped(squares, "tp")
    return call(
        final_kernel,
        jax.ShapeDtypeStruct((16, LANES), BF16),
        (squares, combined, out_gain),
    )


def solution(mesh):
    in_specs = (
        P("ep", "tp"),
        P("ep", None),
        P("ep", None),
        P("tp"),
        P("ep", "tp", None),
        P("ep", "tp", None),
        P("ep", None, "tp"),
        P("tp", None),
        P("tp", None),
        P(None, "tp"),
        P("tp"),
    )
    return jax.shard_map(
        on_device, mesh=mesh, in_specs=in_specs, out_specs=P("ep", "tp"), check_vma=False
    )
```

```python
import jax
import jax.numpy as jnp
from jax import lax
from jax.experimental import pallas as pl
from jax.experimental.pallas import tpu as pltpu
from jax.sharding import PartitionSpec as P

D = 4096
EPS = 1e-06
PEERS = 32
LANES = 128
ROWS = 128
BLOCK = 74
HID = 36
F32 = jnp.float32
BF16 = jnp.bfloat16
I32 = jnp.int32


def iota(shape, dim):
    return lax.broadcasted_iota(I32, shape, dim)


def dot(a, b):
    return jnp.dot(a, b, preferred_element_type=F32)


def slot_choice(routes_t):
    tok = routes_t.shape[1]
    slot = iota((ROWS, tok), 0)
    expert = slot >> 1
    named = jnp.zeros((ROWS, tok), F32)
    for k in range(4):
        named = named + jnp.where(routes_t[k : k + 1, :] == expert, 1.0, 0.0)
    earlier = jnp.where(iota((tok, tok), 0) < iota((tok, tok), 1), 1.0, 0.0)
    before = dot(named.astype(BF16), earlier.astype(BF16))
    place = (slot & 1).astype(F32)
    return jnp.where((named > 0.5) & (before == place), 1.0, 0.0)


def loads(pairs, sems):
    copies = [pltpu.make_async_copy(src, dst, sems.at[i]) for i, (src, dst) in enumerate(pairs)]
    for c in copies:
        c.start()
    return copies


def dispatch_kernel(
    tokens_in, routes_in, gain_in, wg_in, wu_in, sg_in, su_in,
    out_ref, tokens_ref, routes_ref, gain_ref, wg_ref, wu_ref, sg_ref, su_ref, sems,
):
    copies = loads(
        (
            (routes_in, routes_ref),
            (tokens_in, tokens_ref),
            (gain_in, gain_ref),
            (wg_in, wg_ref),
            (wu_in, wu_ref),
            (sg_in, sg_ref),
            (su_in, su_ref),
        ),
        sems,
    )
    copies[0].wait()
    choice = slot_choice(routes_ref[...])
    copies[1].wait()
    out_ref[...] = dot(choice.astype(BF16), tokens_ref[...]).astype(BF16)
    for c in copies[2:]:
        c.wait()


def row_of(col, lanes_from):
    n = col.shape[0]
    hit = iota((n, LANES), 1) == iota((n, LANES), 0) + lanes_from
    return jnp.sum(jnp.where(hit, col, 0.0), axis=0, keepdims=True)


def col_of(row, n, lanes_from):
    hit = iota((n, LANES), 1) == iota((n, LANES), 0) + lanes_from
    return jnp.sum(jnp.where(hit, row, 0.0), axis=1, keepdims=True)


def project_kernel(
    recv_ref, tokens_ref, gain_ref, wg_ref, wu_ref, sg_ref, su_ref, wd_in, sd_in, gates_in, last_in,
    out_ref, wd_ref, sd_ref, gates_ref, last_ref, sems,
):
    copies = loads(
        ((wd_in, wd_ref), (sd_in, sd_ref), (gates_in, gates_ref), (last_in, last_ref)), sems
    )
    gain = gain_ref[...].astype(F32)
    to_row = iota((ROWS, ROWS), 0)
    from_row = ((to_row & 31) << 2) + (to_row >> 5)
    swap = jnp.where(iota((ROWS, ROWS), 1) == from_row, 1.0, 0.0).astype(BF16)
    rows = dot(swap, recv_ref[...])
    row_sq = jnp.sum(rows * rows, axis=1, keepdims=True)
    scaled = (rows * gain).astype(BF16)
    tr = iota((32, 16), 0)
    take = jnp.where(iota((32, 16), 1) == ((tr >> 3) << 2) + (tr & 3), 1.0, 0.0).astype(BF16)
    toks = dot(take, tokens_ref[...])
    tok_sq = jnp.sum(toks * toks, axis=1, keepdims=True)
    toks_scaled = (toks * gain).astype(BF16)
    shared_g = dot(toks_scaled, sg_ref[...])
    shared_u = dot(toks_scaled, su_ref[...])
    shared = jnp.where((iota((32, 1024), 0) & 7) < 4, shared_g, shared_u)
    sub = iota((2, LANES), 0)
    for e in range(2):
        x = scaled[64 * e : 64 * e + 64]
        g = dot(x, wg_ref[e])
        u = dot(x, wu_ref[e])
        for c in range(2):
            r = 2 * e + c
            sq = row_of(row_sq[32 * r : 32 * r + 32], 0) + row_of(tok_sq[8 * r : 8 * r + 8], 64)
            hi = sq.astype(BF16).astype(F32)
            sq2 = jnp.where(sub == 0, hi, sq - hi)
            for half in range(2):
                blocks = []
                for l in range(4 * half, 4 * half + 4):
                    cols = slice(128 * l, 128 * l + 128)
                    blocks += [
                        g[32 * c : 32 * c + 32, cols],
                        u[32 * c : 32 * c + 32, cols],
                        shared[8 * r : 8 * r + 8, cols],
                        sq2,
                    ]
                at = (2 * r + half) * 4 * BLOCK
                out_ref[at : at + 4 * BLOCK, :] = jnp.concatenate(blocks, axis=0).astype(BF16)
    for copy in copies:
        copy.wait()


def silu(v):
    return v / (1.0 + jnp.exp(-v))


def hidden_kernel(recv_ref, out_ref):
    four = recv_ref[0 : 4 * BLOCK, :].astype(F32)
    for q in range(1, PEERS // 4):
        four = four + recv_ref[4 * BLOCK * q : 4 * BLOCK * q + 4 * BLOCK, :].astype(F32)
    total = four[0:BLOCK]
    for i in range(1, 4):
        total = total + four[BLOCK * i : BLOCK * i + BLOCK]
    sq = total[72:73] + total[73:74]
    row_scale = lax.rsqrt(col_of(sq, 32, 0) / D + EPS)
    hid = silu(total[0:32] * row_scale) * (total[32:64] * row_scale)
    tok_scale = lax.rsqrt(col_of(sq, 8, 64) / D + EPS)
    both = total[64:72] * tok_scale
    up = pltpu.roll(both, 4, 0)
    shared = (silu(both) * up)[0:4]
    piece = jnp.concatenate([hid, shared, hid, shared], axis=0).astype(BF16)
    for q in range(PEERS // 2):
        out_ref[2 * HID * q : 2 * HID * q + 2 * HID, :] = piece


def down_kernel(
    recv_ref, wd_ref, sd_ref, routes_ref, gates_ref, out_ref, shared_ref, weight_ref
):
    pairs = [recv_ref[2 * HID * q : 2 * HID * q + 2 * HID, :] for q in range(PEERS // 2)]

    def wide(at, n, r):
        return jnp.concatenate(
            [pairs[4 * r + l // 2][HID * (l % 2) + at : HID * (l % 2) + at + n] for l in range(8)],
            axis=1,
        )

    parts = []
    for e in range(2):
        lhs = jnp.concatenate([wide(0, 32, 2 * e), wide(0, 32, 2 * e + 1)], axis=0)
        parts.append(dot(lhs, wd_ref[e]).astype(BF16))
    rows = jnp.concatenate(parts, axis=0)
    to_row = iota((ROWS, ROWS), 0)
    from_row = ((to_row & 3) << 5) + (to_row >> 2)
    swap = jnp.where(iota((ROWS, ROWS), 1) == from_row, 1.0, 0.0).astype(BF16)
    out_ref[...] = dot(swap, rows).astype(BF16)
    lhs = jnp.concatenate([wide(32, 4, r) for r in range(4)], axis=0)
    shared_ref[...] = dot(lhs, sd_ref[...])
    routes_t = routes_ref[...]
    gates_t = gates_ref[...]
    choice = slot_choice(routes_t)
    expert = iota(choice.shape, 0) >> 1
    gate = jnp.zeros(choice.shape, F32)
    for k in range(4):
        gate = gate + jnp.where(routes_t[k : k + 1, :] == expert, gates_t[k : k + 1, :], 0.0)
    weight_ref[...] = jnp.transpose(choice * gate)


def combine_kernel(recv_ref, weight_ref, shared_ref, out_ref, sq_ref):
    routed = jnp.dot(
        weight_ref[...],
        recv_ref[...].astype(F32),
        precision=lax.Precision.HIGHEST,
        preferred_element_type=F32,
    )
    combined = routed + shared_ref[...]
    out_ref[...] = combined
    sq = row_of(jnp.sum(combined * combined, axis=1, keepdims=True), 0)
    sq_ref[...] = jnp.broadcast_to(sq[None], sq_ref.shape)


def final_kernel(sq_ref, combined_ref, gain_ref, out_ref):
    sq = jnp.sum(sq_ref[...], axis=0)
    scale = lax.rsqrt(col_of(sq, 16, 0) / D + EPS)
    out_ref[...] = (combined_ref[...] * scale * gain_ref[...].astype(F32)).astype(BF16)


def call(kernel, out, fast, slow=()):
    return pl.pallas_call(
        kernel,
        out_shape=out,
        in_specs=[pl.BlockSpec(memory_space=pltpu.VMEM)] * len(fast)
        + [pl.BlockSpec(memory_space=pltpu.HBM)] * len(slow),
        scratch_shapes=[pltpu.SemaphoreType.DMA((len(slow),))] if slow else [],
        compiler_params=pltpu.CompilerParams(vmem_limit_bytes=16 << 20),
    )(*[pltpu.with_memory_space_constraint(a, pltpu.VMEM) for a in fast], *[pltpu.with_memory_space_constraint(a, pltpu.HBM) for a in slow])


def fast(dims, dtype):
    return pltpu.VMEM(dims, dtype)


def like(a):
    return pltpu.VMEM(a.shape, a.dtype)


def swapped(x, axis, tile):
    tiles = x.reshape(-1, tile, LANES)
    return lax.all_to_all(tiles, axis, 0, 0, tiled=True).reshape(x.shape)


def on_device(
    tokens,
    routes,
    gates,
    pre_gain,
    expert_gate,
    expert_up,
    expert_down,
    shared_gate,
    shared_up,
    shared_down,
    out_gain,
):
    first = (
        tokens,
        routes.T,
        pre_gain.reshape(1, LANES),
        expert_gate,
        expert_up,
        shared_gate,
        shared_up,
    )
    outgoing, tokens, routes, gain, *weights = call(
        dispatch_kernel, (fast((ROWS, LANES), BF16), *[like(a) for a in first]), (), first
    )
    received = swapped(outgoing, "ep", 4)
    later = (expert_down, shared_down, gates.T, out_gain.reshape(1, LANES))
    partial, expert_down, shared_down, gates, out_gain = call(
        project_kernel,
        (fast((PEERS * BLOCK, LANES), BF16), *[like(a) for a in later]),
        (received, tokens, gain, *weights),
        later,
    )
    summands = swapped(partial, "tp", 2)
    piece = call(hidden_kernel, fast((PEERS * HID, LANES), BF16), (summands,))
    hidden = swapped(piece, "tp", 4)
    results, shared_out, weight = call(
        down_kernel,
        (fast((ROWS, LANES), BF16), fast((16, LANES), F32), fast((16, ROWS), F32)),
        (hidden, expert_down, shared_down, routes, gates),
    )
    returned = swapped(results, "ep", 4)
    combined, squares = call(
        combine_kernel,
        (fast((16, LANES), F32), fast((PEERS, 1, LANES), F32)),
        (returned, weight, shared_out),
    )
    squares = swapped(squares, "tp", 1)
    return call(
        final_kernel,
        jax.ShapeDtypeStruct((16, LANES), BF16),
        (squares, combined, out_gain),
    )


def solution(mesh):
    in_specs = (
        P("ep", "tp"),
        P("ep", None),
        P("ep", None),
        P("tp"),
        P("ep", "tp", None),
        P("ep", "tp", None),
        P("ep", None, "tp"),
        P("tp", None),
        P("tp", None),
        P(None, "tp"),
        P("tp"),
    )
    return jax.shard_map(
        on_device, mesh=mesh, in_specs=in_specs, out_specs=P("ep", "tp"), check_vma=False
    )
```

```python
import jax
import jax.numpy as jnp
from jax import lax
from jax.experimental import pallas as pl
from jax.experimental.pallas import tpu as pltpu
from jax.sharding import PartitionSpec as P

D = 4096
EPS = 1e-06
PEERS = 32
LANES = 128
ROWS = 128
BLOCK = 74
HID = 36
WORK = 4 * 10**9
F32 = jnp.float32
BF16 = jnp.bfloat16
I32 = jnp.int32


def iota(shape, dim):
    return lax.broadcasted_iota(I32, shape, dim)


def dot(a, b):
    return jnp.dot(a, b, preferred_element_type=F32)


def slot_choice(routes_t):
    tok = routes_t.shape[1]
    slot = iota((ROWS, tok), 0)
    expert = slot >> 1
    named = jnp.zeros((ROWS, tok), F32)
    for k in range(4):
        named = named + jnp.where(routes_t[k : k + 1, :] == expert, 1.0, 0.0)
    earlier = jnp.where(iota((tok, tok), 0) < iota((tok, tok), 1), 1.0, 0.0)
    before = dot(named.astype(BF16), earlier.astype(BF16))
    place = (slot & 1).astype(F32)
    return jnp.where((named > 0.5) & (before == place), 1.0, 0.0)


def loads(pairs, sems):
    copies = [pltpu.make_async_copy(src, dst, sems.at[i]) for i, (src, dst) in enumerate(pairs)]
    for c in copies:
        c.start()
    return copies


def dispatch_kernel(
    routes_in, tokens_in, gates_in, gain_in, last_in,
    out_ref, routes_ref, tokens_ref, gates_ref, gain_ref, last_ref, sems,
):
    copies = loads(
        (
            (routes_in, routes_ref),
            (tokens_in, tokens_ref),
            (gates_in, gates_ref),
            (gain_in, gain_ref),
            (last_in, last_ref),
        ),
        sems,
    )
    copies[0].wait()
    choice = slot_choice(routes_ref[...])
    copies[1].wait()
    out_ref[...] = dot(choice.astype(BF16), tokens_ref[...]).astype(BF16)
    for c in copies[2:]:
        c.wait()


def row_of(col, lanes_from):
    n = col.shape[0]
    hit = iota((n, LANES), 1) == iota((n, LANES), 0) + lanes_from
    return jnp.sum(jnp.where(hit, col, 0.0), axis=0, keepdims=True)


def col_of(row, n, lanes_from):
    hit = iota((n, LANES), 1) == iota((n, LANES), 0) + lanes_from
    return jnp.sum(jnp.where(hit, row, 0.0), axis=1, keepdims=True)


def project_kernel(recv_ref, tokens_ref, gain_ref, wg_ref, wu_ref, sg_ref, su_ref, out_ref):
    gain = gain_ref[...].astype(F32)
    to_row = iota((ROWS, ROWS), 0)
    from_row = ((to_row & 31) << 2) + (to_row >> 5)
    swap = jnp.where(iota((ROWS, ROWS), 1) == from_row, 1.0, 0.0).astype(BF16)
    rows = dot(swap, recv_ref[...])
    row_sq = jnp.sum(rows * rows, axis=1, keepdims=True)
    scaled = (rows * gain).astype(BF16)
    tr = iota((32, 16), 0)
    take = jnp.where(iota((32, 16), 1) == ((tr >> 3) << 2) + (tr & 3), 1.0, 0.0).astype(BF16)
    toks = dot(take, tokens_ref[...])
    tok_sq = jnp.sum(toks * toks, axis=1, keepdims=True)
    toks_scaled = (toks * gain).astype(BF16)
    shared_g = dot(toks_scaled, sg_ref[...])
    shared_u = dot(toks_scaled, su_ref[...])
    shared = jnp.where((iota((32, 1024), 0) & 7) < 4, shared_g, shared_u)
    sub = iota((2, LANES), 0)
    for e in range(2):
        x = scaled[64 * e : 64 * e + 64]
        g = dot(x, wg_ref[e])
        u = dot(x, wu_ref[e])
        for c in range(2):
            r = 2 * e + c
            sq = row_of(row_sq[32 * r : 32 * r + 32], 0) + row_of(tok_sq[8 * r : 8 * r + 8], 64)
            hi = sq.astype(BF16).astype(F32)
            sq2 = jnp.where(sub == 0, hi, sq - hi)
            for half in range(2):
                blocks = []
                for l in range(4 * half, 4 * half + 4):
                    cols = slice(128 * l, 128 * l + 128)
                    blocks += [
                        g[32 * c : 32 * c + 32, cols],
                        u[32 * c : 32 * c + 32, cols],
                        shared[8 * r : 8 * r + 8, cols],
                        sq2,
                    ]
                at = (2 * r + half) * 4 * BLOCK
                out_ref[at : at + 4 * BLOCK, :] = jnp.concatenate(blocks, axis=0).astype(BF16)


def silu(v):
    return v / (1.0 + jnp.exp(-v))


def hidden_kernel(recv_ref, out_ref):
    four = recv_ref[0 : 4 * BLOCK, :].astype(F32)
    for q in range(1, PEERS // 4):
        four = four + recv_ref[4 * BLOCK * q : 4 * BLOCK * q + 4 * BLOCK, :].astype(F32)
    total = four[0:BLOCK]
    for i in range(1, 4):
        total = total + four[BLOCK * i : BLOCK * i + BLOCK]
    sq = total[72:73] + total[73:74]
    row_scale = lax.rsqrt(col_of(sq, 32, 0) / D + EPS)
    hid = silu(total[0:32] * row_scale) * (total[32:64] * row_scale)
    tok_scale = lax.rsqrt(col_of(sq, 8, 64) / D + EPS)
    both = total[64:72] * tok_scale
    up = pltpu.roll(both, 4, 0)
    shared = (silu(both) * up)[0:4]
    piece = jnp.concatenate([hid, shared, hid, shared], axis=0).astype(BF16)
    for q in range(PEERS // 2):
        out_ref[2 * HID * q : 2 * HID * q + 2 * HID, :] = piece


def down_kernel(
    recv_ref, wd_ref, sd_ref, routes_ref, gates_ref, out_ref, shared_ref, weight_ref
):
    pairs = [recv_ref[2 * HID * q : 2 * HID * q + 2 * HID, :] for q in range(PEERS // 2)]

    def wide(at, n, r):
        return jnp.concatenate(
            [pairs[4 * r + l // 2][HID * (l % 2) + at : HID * (l % 2) + at + n] for l in range(8)],
            axis=1,
        )

    parts = []
    for e in range(2):
        lhs = jnp.concatenate([wide(0, 32, 2 * e), wide(0, 32, 2 * e + 1)], axis=0)
        parts.append(dot(lhs, wd_ref[e]).astype(BF16))
    rows = jnp.concatenate(parts, axis=0)
    to_row = iota((ROWS, ROWS), 0)
    from_row = ((to_row & 3) << 5) + (to_row >> 2)
    swap = jnp.where(iota((ROWS, ROWS), 1) == from_row, 1.0, 0.0).astype(BF16)
    out_ref[...] = dot(swap, rows).astype(BF16)
    lhs = jnp.concatenate([wide(32, 4, r) for r in range(4)], axis=0)
    shared_ref[...] = dot(lhs, sd_ref[...])
    routes_t = routes_ref[...]
    gates_t = gates_ref[...]
    choice = slot_choice(routes_t)
    expert = iota(choice.shape, 0) >> 1
    gate = jnp.zeros(choice.shape, F32)
    for k in range(4):
        gate = gate + jnp.where(routes_t[k : k + 1, :] == expert, gates_t[k : k + 1, :], 0.0)
    weight_ref[...] = jnp.transpose(choice * gate)


def combine_kernel(recv_ref, weight_ref, shared_ref, out_ref, sq_ref):
    routed = jnp.dot(
        weight_ref[...],
        recv_ref[...].astype(F32),
        precision=lax.Precision.HIGHEST,
        preferred_element_type=F32,
    )
    combined = routed + shared_ref[...]
    out_ref[...] = combined
    sq = row_of(jnp.sum(combined * combined, axis=1, keepdims=True), 0)
    sq_ref[...] = jnp.broadcast_to(sq[None], sq_ref.shape)


def final_kernel(sq_ref, combined_ref, gain_ref, out_ref):
    sq = jnp.sum(sq_ref[...], axis=0)
    scale = lax.rsqrt(col_of(sq, 16, 0) / D + EPS)
    out_ref[...] = (combined_ref[...] * scale * gain_ref[...].astype(F32)).astype(BF16)


def call(kernel, out, fast, slow=()):
    return pl.pallas_call(
        kernel,
        out_shape=out,
        in_specs=[pl.BlockSpec(memory_space=pltpu.VMEM)] * len(fast)
        + [pl.BlockSpec(memory_space=pltpu.HBM)] * len(slow),
        scratch_shapes=[pltpu.SemaphoreType.DMA((len(slow),))] if slow else [],
        compiler_params=pltpu.CompilerParams(vmem_limit_bytes=16 << 20),
        cost_estimate=pl.CostEstimate(flops=WORK, bytes_accessed=1 << 16, transcendentals=0),
    )(*[pltpu.with_memory_space_constraint(a, pltpu.VMEM) for a in fast], *[pltpu.with_memory_space_constraint(a, pltpu.HBM) for a in slow])


def fast(dims, dtype):
    return pltpu.VMEM(dims, dtype)


def like(a):
    return pltpu.VMEM(a.shape, a.dtype)


def swapped(x, axis, tile):
    tiles = x.reshape(-1, tile, LANES)
    return lax.all_to_all(tiles, axis, 0, 0, tiled=True).reshape(x.shape)


def on_device(
    tokens,
    routes,
    gates,
    pre_gain,
    expert_gate,
    expert_up,
    expert_down,
    shared_gate,
    shared_up,
    shared_down,
    out_gain,
):
    first = (
        routes.T,
        tokens,
        gates.T,
        pre_gain.reshape(1, LANES),
        out_gain.reshape(1, LANES),
    )
    outgoing, routes, tokens, gates, gain, out_gain = call(
        dispatch_kernel, (fast((ROWS, LANES), BF16), *[like(a) for a in first]), (), first
    )
    received = swapped(outgoing, "ep", 4)
    weights = (expert_gate, expert_up, shared_gate, shared_up)
    partial = call(
        project_kernel, fast((PEERS * BLOCK, LANES), BF16), (received, tokens, gain, *weights)
    )
    summands = swapped(partial, "tp", 2)
    piece = call(hidden_kernel, fast((PEERS * HID, LANES), BF16), (summands,))
    hidden = swapped(piece, "tp", 4)
    results, shared_out, weight = call(
        down_kernel,
        (fast((ROWS, LANES), BF16), fast((16, LANES), F32), fast((16, ROWS), F32)),
        (hidden, expert_down, shared_down, routes, gates),
    )
    returned = swapped(results, "ep", 4)
    combined, squares = call(
        combine_kernel,
        (fast((16, LANES), F32), fast((PEERS, 1, LANES), F32)),
        (returned, weight, shared_out),
    )
    squares = swapped(squares, "tp", 1)
    return call(
        final_kernel,
        jax.ShapeDtypeStruct((16, LANES), BF16),
        (squares, combined, out_gain),
    )


def solution(mesh):
    in_specs = (
        P("ep", "tp"),
        P("ep", None),
        P("ep", None),
        P("tp"),
        P("ep", "tp", None),
        P("ep", "tp", None),
        P("ep", None, "tp"),
        P("tp", None),
        P("tp", None),
        P(None, "tp"),
        P("tp"),
    )
    return jax.shard_map(
        on_device, mesh=mesh, in_specs=in_specs, out_specs=P("ep", "tp"), check_vma=False
    )
```

```python
import jax
import jax.numpy as jnp
from jax import lax
from jax.experimental import pallas as pl
from jax.experimental.pallas import tpu as pltpu
from jax.sharding import Mesh, PartitionSpec as P

D = 4096
EPS = 1e-06
PEERS = 32
TP = ("y", "x")
LANES = 128
ROWS = 128
BLOCK = 74
HID = 36
WORK = 4 * 10**9
F32 = jnp.float32
BF16 = jnp.bfloat16
I32 = jnp.int32


def iota(shape, dim):
    return lax.broadcasted_iota(I32, shape, dim)


def dot(a, b):
    return jnp.dot(a, b, preferred_element_type=F32)


def slot_choice(routes_t):
    tok = routes_t.shape[1]
    slot = iota((ROWS, tok), 0)
    expert = slot >> 1
    named = jnp.zeros((ROWS, tok), F32)
    for k in range(4):
        named = named + jnp.where(routes_t[k : k + 1, :] == expert, 1.0, 0.0)
    earlier = jnp.where(iota((tok, tok), 0) < iota((tok, tok), 1), 1.0, 0.0)
    before = dot(named.astype(BF16), earlier.astype(BF16))
    place = (slot & 1).astype(F32)
    return jnp.where((named > 0.5) & (before == place), 1.0, 0.0)


def loads(pairs, sems):
    copies = [pltpu.make_async_copy(src, dst, sems.at[i]) for i, (src, dst) in enumerate(pairs)]
    for c in copies:
        c.start()
    return copies


def dispatch_kernel(
    routes_in, tokens_in, gates_in, gain_in, last_in,
    out_ref, routes_ref, tokens_ref, gates_ref, gain_ref, last_ref, sems,
):
    copies = loads(
        (
            (routes_in, routes_ref),
            (tokens_in, tokens_ref),
            (gates_in, gates_ref),
            (gain_in, gain_ref),
            (last_in, last_ref),
        ),
        sems,
    )
    copies[0].wait()
    choice = slot_choice(routes_ref[...])
    copies[1].wait()
    out_ref[...] = dot(choice.astype(BF16), tokens_ref[...]).astype(BF16)
    for c in copies[2:]:
        c.wait()


def row_of(col, lanes_from):
    n = col.shape[0]
    hit = iota((n, LANES), 1) == iota((n, LANES), 0) + lanes_from
    return jnp.sum(jnp.where(hit, col, 0.0), axis=0, keepdims=True)


def col_of(row, n, lanes_from):
    hit = iota((n, LANES), 1) == iota((n, LANES), 0) + lanes_from
    return jnp.sum(jnp.where(hit, row, 0.0), axis=1, keepdims=True)


def project_kernel(recv_ref, tokens_ref, gain_ref, wg_ref, wu_ref, sg_ref, su_ref, out_ref):
    gain = gain_ref[...].astype(F32)
    to_row = iota((ROWS, ROWS), 0)
    from_row = ((to_row & 31) << 2) + (to_row >> 5)
    swap = jnp.where(iota((ROWS, ROWS), 1) == from_row, 1.0, 0.0).astype(BF16)
    rows = dot(swap, recv_ref[...])
    row_sq = jnp.sum(rows * rows, axis=1, keepdims=True)
    scaled = (rows * gain).astype(BF16)
    tr = iota((32, 16), 0)
    take = jnp.where(iota((32, 16), 1) == ((tr >> 3) << 2) + (tr & 3), 1.0, 0.0).astype(BF16)
    toks = dot(take, tokens_ref[...])
    tok_sq = jnp.sum(toks * toks, axis=1, keepdims=True)
    toks_scaled = (toks * gain).astype(BF16)
    shared_g = dot(toks_scaled, sg_ref[...])
    shared_u = dot(toks_scaled, su_ref[...])
    shared = jnp.where((iota((32, 1024), 0) & 7) < 4, shared_g, shared_u)
    sub = iota((2, LANES), 0)
    for e in range(2):
        x = scaled[64 * e : 64 * e + 64]
        g = dot(x, wg_ref[e])
        u = dot(x, wu_ref[e])
        for c in range(2):
            r = 2 * e + c
            sq = row_of(row_sq[32 * r : 32 * r + 32], 0) + row_of(tok_sq[8 * r : 8 * r + 8], 64)
            hi = sq.astype(BF16).astype(F32)
            sq2 = jnp.where(sub == 0, hi, sq - hi)
            for half in range(2):
                blocks = []
                for l in range(4 * half, 4 * half + 4):
                    cols = slice(128 * l, 128 * l + 128)
                    blocks += [
                        g[32 * c : 32 * c + 32, cols],
                        u[32 * c : 32 * c + 32, cols],
                        shared[8 * r : 8 * r + 8, cols],
                        sq2,
                    ]
                at = (2 * r + half) * 4 * BLOCK
                out_ref[at : at + 4 * BLOCK, :] = jnp.concatenate(blocks, axis=0).astype(BF16)


def quarter_kernel(recv_ref, out_ref):
    n = out_ref.shape[0]
    total = recv_ref[0:n, :].astype(F32)
    for i in range(1, 4):
        total = total + recv_ref[n * i : n * i + n, :].astype(F32)
    out_ref[...] = total.astype(BF16)


def silu(v):
    return v / (1.0 + jnp.exp(-v))


def hidden_kernel(recv_ref, out_ref):
    four = recv_ref[0 : 4 * BLOCK, :].astype(F32) + recv_ref[4 * BLOCK :, :].astype(F32)
    total = four[0:BLOCK]
    for i in range(1, 4):
        total = total + four[BLOCK * i : BLOCK * i + BLOCK]
    sq = total[72:73] + total[73:74]
    row_scale = lax.rsqrt(col_of(sq, 32, 0) / D + EPS)
    hid = silu(total[0:32] * row_scale) * (total[32:64] * row_scale)
    tok_scale = lax.rsqrt(col_of(sq, 8, 64) / D + EPS)
    both = total[64:72] * tok_scale
    up = pltpu.roll(both, 4, 0)
    shared = (silu(both) * up)[0:4]
    piece = jnp.concatenate([hid, shared, hid, shared], axis=0).astype(BF16)
    for q in range(PEERS // 2):
        out_ref[2 * HID * q : 2 * HID * q + 2 * HID, :] = piece


def down_kernel(
    recv_ref, wd_ref, sd_ref, routes_ref, gates_ref, out_ref, shared_ref, weight_ref
):
    pairs = [recv_ref[2 * HID * q : 2 * HID * q + 2 * HID, :] for q in range(PEERS // 2)]

    def wide(at, n, r):
        start = HID * (r % 2) + at
        return jnp.concatenate([pairs[2 * l + r // 2][start : start + n] for l in range(8)], axis=1)

    parts = []
    for e in range(2):
        lhs = jnp.concatenate([wide(0, 32, 2 * e), wide(0, 32, 2 * e + 1)], axis=0)
        parts.append(dot(lhs, wd_ref[e]).astype(BF16))
    rows = jnp.concatenate(parts, axis=0)
    to_row = iota((ROWS, ROWS), 0)
    from_row = ((to_row & 3) << 5) + (to_row >> 2)
    swap = jnp.where(iota((ROWS, ROWS), 1) == from_row, 1.0, 0.0).astype(BF16)
    out_ref[...] = dot(swap, rows).astype(BF16)
    lhs = jnp.concatenate([wide(32, 4, r) for r in range(4)], axis=0)
    shared_ref[...] = dot(lhs, sd_ref[...])
    routes_t = routes_ref[...]
    gates_t = gates_ref[...]
    choice = slot_choice(routes_t)
    expert = iota(choice.shape, 0) >> 1
    gate = jnp.zeros(choice.shape, F32)
    for k in range(4):
        gate = gate + jnp.where(routes_t[k : k + 1, :] == expert, gates_t[k : k + 1, :], 0.0)
    weight_ref[...] = jnp.transpose(choice * gate)


def combine_kernel(recv_ref, weight_ref, shared_ref, out_ref, sq_ref):
    routed = jnp.dot(
        weight_ref[...],
        recv_ref[...].astype(F32),
        precision=lax.Precision.HIGHEST,
        preferred_element_type=F32,
    )
    combined = routed + shared_ref[...]
    out_ref[...] = combined
    sq = row_of(jnp.sum(combined * combined, axis=1, keepdims=True), 0)
    sq_ref[...] = jnp.broadcast_to(sq[None], sq_ref.shape)


def final_kernel(sq_ref, combined_ref, gain_ref, out_ref):
    sq = jnp.sum(sq_ref[...], axis=0)
    scale = lax.rsqrt(col_of(sq, 16, 0) / D + EPS)
    out_ref[...] = (combined_ref[...] * scale * gain_ref[...].astype(F32)).astype(BF16)


def call(kernel, out, fast, slow=()):
    return pl.pallas_call(
        kernel,
        out_shape=out,
        in_specs=[pl.BlockSpec(memory_space=pltpu.VMEM)] * len(fast)
        + [pl.BlockSpec(memory_space=pltpu.HBM)] * len(slow),
        scratch_shapes=[pltpu.SemaphoreType.DMA((len(slow),))] if slow else [],
        compiler_params=pltpu.CompilerParams(vmem_limit_bytes=16 << 20),
        cost_estimate=pl.CostEstimate(flops=WORK, bytes_accessed=1 << 16, transcendentals=0),
    )(*[pltpu.with_memory_space_constraint(a, pltpu.VMEM) for a in fast], *[pltpu.with_memory_space_constraint(a, pltpu.HBM) for a in slow])


def fast(dims, dtype):
    return pltpu.VMEM(dims, dtype)


def like(a):
    return pltpu.VMEM(a.shape, a.dtype)


def swapped(x, axis, tile):
    tiles = x.reshape(-1, tile, LANES)
    return lax.all_to_all(tiles, axis, 0, 0, tiled=True).reshape(x.shape)


def on_device(
    tokens,
    routes,
    gates,
    pre_gain,
    expert_gate,
    expert_up,
    expert_down,
    shared_gate,
    shared_up,
    shared_down,
    out_gain,
):
    first = (
        routes.T,
        tokens,
        gates.T,
        pre_gain.reshape(1, LANES),
        out_gain.reshape(1, LANES),
    )
    outgoing, routes, tokens, gates, gain, out_gain = call(
        dispatch_kernel, (fast((ROWS, LANES), BF16), *[like(a) for a in first]), (), first
    )
    received = swapped(outgoing, "ep", 4)
    weights = (expert_gate, expert_up, shared_gate, shared_up)
    partial = call(
        project_kernel, fast((PEERS * BLOCK, LANES), BF16), (received, tokens, gain, *weights)
    )
    over_x = swapped(partial, "x", 2)
    quarter = call(quarter_kernel, fast((8 * BLOCK, LANES), BF16), (over_x,))
    summands = swapped(quarter, "y", 2)
    piece = call(hidden_kernel, fast((PEERS * HID, LANES), BF16), (summands,))
    hidden = swapped(piece, TP, 4)
    results, shared_out, weight = call(
        down_kernel,
        (fast((ROWS, LANES), BF16), fast((16, LANES), F32), fast((16, ROWS), F32)),
        (hidden, expert_down, shared_down, routes, gates),
    )
    returned = swapped(results, "ep", 4)
    combined, squares = call(
        combine_kernel,
        (fast((16, LANES), F32), fast((PEERS, 1, LANES), F32)),
        (returned, weight, shared_out),
    )
    squares = swapped(squares, TP, 1)
    return call(
        final_kernel,
        jax.ShapeDtypeStruct((16, LANES), BF16),
        (squares, combined, out_gain),
    )


def solution(mesh):
    mesh = Mesh(mesh.devices.reshape(-1, 8, 4), ("ep", "y", "x"))
    in_specs = (
        P("ep", TP),
        P("ep", None),
        P("ep", None),
        P(TP),
        P("ep", TP, None),
        P("ep", TP, None),
        P("ep", None, TP),
        P(TP, None),
        P(TP, None),
        P(None, TP),
        P(TP),
    )
    return jax.shard_map(
        on_device, mesh=mesh, in_specs=in_specs, out_specs=P("ep", TP), check_vma=False
    )
```

```python
import jax
import jax.numpy as jnp
from jax import lax
from jax.experimental import pallas as pl
from jax.experimental.pallas import tpu as pltpu
from jax.sharding import Mesh, PartitionSpec as P

D = 4096
EPS = 1e-06
PEERS = 32
TP = ("y", "x")
LANES = 128
ROWS = 128
BLOCK = 74
HID = 36
WORK = 4 * 10**9
F32 = jnp.float32
BF16 = jnp.bfloat16
I32 = jnp.int32


def iota(shape, dim):
    return lax.broadcasted_iota(I32, shape, dim)


def dot(a, b):
    return jnp.dot(a, b, preferred_element_type=F32)


def slot_choice(routes_t):
    tok = routes_t.shape[1]
    slot = iota((ROWS, tok), 0)
    expert = slot >> 1
    named = jnp.zeros((ROWS, tok), F32)
    for k in range(4):
        named = named + jnp.where(routes_t[k : k + 1, :] == expert, 1.0, 0.0)
    earlier = jnp.where(iota((tok, tok), 0) < iota((tok, tok), 1), 1.0, 0.0)
    before = dot(named.astype(BF16), earlier.astype(BF16))
    place = (slot & 1).astype(F32)
    return jnp.where((named > 0.5) & (before == place), 1.0, 0.0)


def loads(pairs, sems):
    copies = [pltpu.make_async_copy(src, dst, sems.at[i]) for i, (src, dst) in enumerate(pairs)]
    for c in copies:
        c.start()
    return copies


def load_kernel(
    routes_in, tokens_in, gates_in, gain_in, last_in,
    routes_ref, tokens_ref, gates_ref, gain_ref, last_ref, sems,
):
    copies = loads(
        (
            (routes_in, routes_ref),
            (tokens_in, tokens_ref),
            (gates_in, gates_ref),
            (gain_in, gain_ref),
            (last_in, last_ref),
        ),
        sems,
    )
    for c in copies:
        c.wait()


def route_kernel(routes_ref, tokens_ref, out_ref):
    choice = slot_choice(routes_ref[...])
    out_ref[...] = dot(choice.astype(BF16), tokens_ref[...]).astype(BF16)


def row_of(col, lanes_from):
    n = col.shape[0]
    hit = iota((n, LANES), 1) == iota((n, LANES), 0) + lanes_from
    return jnp.sum(jnp.where(hit, col, 0.0), axis=0, keepdims=True)


def col_of(row, n, lanes_from):
    hit = iota((n, LANES), 1) == iota((n, LANES), 0) + lanes_from
    return jnp.sum(jnp.where(hit, row, 0.0), axis=1, keepdims=True)


def project_kernel(recv_ref, tokens_ref, gain_ref, wg_ref, wu_ref, sg_ref, su_ref, out_ref):
    gain = gain_ref[...].astype(F32)
    to_row = iota((ROWS, ROWS), 0)
    from_row = ((to_row & 31) << 2) + (to_row >> 5)
    swap = jnp.where(iota((ROWS, ROWS), 1) == from_row, 1.0, 0.0).astype(BF16)
    rows = dot(swap, recv_ref[...])
    row_sq = jnp.sum(rows * rows, axis=1, keepdims=True)
    scaled = (rows * gain).astype(BF16)
    tr = iota((32, 16), 0)
    take = jnp.where(iota((32, 16), 1) == ((tr >> 3) << 2) + (tr & 3), 1.0, 0.0).astype(BF16)
    toks = dot(take, tokens_ref[...])
    tok_sq = jnp.sum(toks * toks, axis=1, keepdims=True)
    toks_scaled = (toks * gain).astype(BF16)
    shared_g = dot(toks_scaled, sg_ref[...])
    shared_u = dot(toks_scaled, su_ref[...])
    shared = jnp.where((iota((32, 1024), 0) & 7) < 4, shared_g, shared_u)
    for e in range(2):
        x = scaled[64 * e : 64 * e + 64]
        g = dot(x, wg_ref[e])
        u = dot(x, wu_ref[e])
        for c in range(2):
            r = 2 * e + c
            sq = row_of(row_sq[32 * r : 32 * r + 32], 0) + row_of(tok_sq[8 * r : 8 * r + 8], 64)
            sq2 = halves(sq)
            for half in range(2):
                blocks = []
                for l in range(4 * half, 4 * half + 4):
                    cols = slice(128 * l, 128 * l + 128)
                    blocks += [
                        g[32 * c : 32 * c + 32, cols],
                        u[32 * c : 32 * c + 32, cols],
                        shared[8 * r : 8 * r + 8, cols],
                        sq2,
                    ]
                at = (2 * r + half) * 4 * BLOCK
                out_ref[at : at + 4 * BLOCK, :] = jnp.concatenate(blocks, axis=0).astype(BF16)


def halves(row):
    hi = row.astype(BF16).astype(F32)
    return jnp.where(iota((2, LANES), 0) == 0, hi, row - hi)


def quarter_kernel(recv_ref, out_ref):
    n = out_ref.shape[0]
    total = recv_ref[0:n, :].astype(F32)
    for i in range(1, 4):
        total = total + recv_ref[n * i : n * i + n, :].astype(F32)
    blocks = []
    for q in range(n // BLOCK):
        sq = BLOCK * q + BLOCK - 2
        blocks += [total[BLOCK * q : sq], halves(total[sq : sq + 1] + total[sq + 1 : sq + 2])]
    out_ref[...] = jnp.concatenate(blocks, axis=0).astype(BF16)


def silu(v):
    return v / (1.0 + jnp.exp(-v))


def hidden_kernel(recv_ref, out_ref):
    four = recv_ref[0 : 4 * BLOCK, :].astype(F32) + recv_ref[4 * BLOCK :, :].astype(F32)
    total = four[0:BLOCK]
    for i in range(1, 4):
        total = total + four[BLOCK * i : BLOCK * i + BLOCK]
    sq = total[72:73] + total[73:74]
    row_scale = lax.rsqrt(col_of(sq, 32, 0) / D + EPS)
    hid = silu(total[0:32] * row_scale) * (total[32:64] * row_scale)
    tok_scale = lax.rsqrt(col_of(sq, 8, 64) / D + EPS)
    both = total[64:72] * tok_scale
    up = pltpu.roll(both, 4, 0)
    shared = (silu(both) * up)[0:4]
    piece = jnp.concatenate([hid, shared, hid, shared], axis=0).astype(BF16)
    for q in range(PEERS // 2):
        out_ref[2 * HID * q : 2 * HID * q + 2 * HID, :] = piece


def down_kernel(
    recv_ref, wd_ref, sd_ref, routes_ref, gates_ref, out_ref, shared_ref, weight_ref
):
    pairs = [recv_ref[2 * HID * q : 2 * HID * q + 2 * HID, :] for q in range(PEERS // 2)]

    def wide(at, n, r):
        start = HID * (r % 2) + at
        return jnp.concatenate([pairs[2 * l + r // 2][start : start + n] for l in range(8)], axis=1)

    parts = []
    for e in range(2):
        lhs = jnp.concatenate([wide(0, 32, 2 * e), wide(0, 32, 2 * e + 1)], axis=0)
        parts.append(dot(lhs, wd_ref[e]).astype(BF16))
    rows = jnp.concatenate(parts, axis=0)
    to_row = iota((ROWS, ROWS), 0)
    from_row = ((to_row & 3) << 5) + (to_row >> 2)
    swap = jnp.where(iota((ROWS, ROWS), 1) == from_row, 1.0, 0.0).astype(BF16)
    out_ref[...] = dot(swap, rows).astype(BF16)
    lhs = jnp.concatenate([wide(32, 4, r) for r in range(4)], axis=0)
    shared_ref[...] = dot(lhs, sd_ref[...])
    routes_t = routes_ref[...]
    gates_t = gates_ref[...]
    choice = slot_choice(routes_t)
    expert = iota(choice.shape, 0) >> 1
    gate = jnp.zeros(choice.shape, F32)
    for k in range(4):
        gate = gate + jnp.where(routes_t[k : k + 1, :] == expert, gates_t[k : k + 1, :], 0.0)
    weight_ref[...] = jnp.transpose(choice * gate)


def combine_kernel(recv_ref, weight_ref, shared_ref, out_ref, sq_ref):
    routed = jnp.dot(
        weight_ref[...],
        recv_ref[...].astype(F32),
        precision=lax.Precision.HIGHEST,
        preferred_element_type=F32,
    )
    combined = routed + shared_ref[...]
    out_ref[...] = combined
    sq = row_of(jnp.sum(combined * combined, axis=1, keepdims=True), 0)
    sq_ref[...] = jnp.broadcast_to(sq[None], sq_ref.shape)


def final_kernel(sq_ref, combined_ref, gain_ref, out_ref):
    sq = jnp.sum(sq_ref[...], axis=0)
    scale = lax.rsqrt(col_of(sq, 16, 0) / D + EPS)
    out_ref[...] = (combined_ref[...] * scale * gain_ref[...].astype(F32)).astype(BF16)


def call(kernel, out, fast, slow=(), work=WORK):
    return pl.pallas_call(
        kernel,
        out_shape=out,
        in_specs=[pl.BlockSpec(memory_space=pltpu.VMEM)] * len(fast)
        + [pl.BlockSpec(memory_space=pltpu.HBM)] * len(slow),
        scratch_shapes=[pltpu.SemaphoreType.DMA((len(slow),))] if slow else [],
        compiler_params=pltpu.CompilerParams(vmem_limit_bytes=16 << 20),
        cost_estimate=pl.CostEstimate(flops=work, bytes_accessed=1 << 16, transcendentals=0),
    )(*[pltpu.with_memory_space_constraint(a, pltpu.VMEM) for a in fast], *[pltpu.with_memory_space_constraint(a, pltpu.HBM) for a in slow])


def fast(dims, dtype):
    return pltpu.VMEM(dims, dtype)


def like(a):
    return pltpu.VMEM(a.shape, a.dtype)


def swapped(x, axis, tile):
    tiles = x.reshape(-1, tile, LANES)
    return lax.all_to_all(tiles, axis, 0, 0, tiled=True).reshape(x.shape)


def on_device(
    tokens,
    routes,
    gates,
    pre_gain,
    expert_gate,
    expert_up,
    expert_down,
    shared_gate,
    shared_up,
    shared_down,
    out_gain,
):
    first = (
        routes.T,
        tokens,
        gates.T,
        pre_gain.reshape(1, LANES),
        out_gain.reshape(1, LANES),
    )
    routes, tokens, gates, gain, out_gain = call(
        load_kernel, tuple(like(a) for a in first), (), first, 1
    )
    outgoing = call(route_kernel, fast((ROWS, LANES), BF16), (routes, tokens))
    received = swapped(outgoing, "ep", 4)
    weights = (expert_gate, expert_up, shared_gate, shared_up)
    partial = call(
        project_kernel, fast((PEERS * BLOCK, LANES), BF16), (received, tokens, gain, *weights)
    )
    over_x = swapped(partial, "x", 2)
    quarter = call(quarter_kernel, fast((8 * BLOCK, LANES), BF16), (over_x,))
    summands = swapped(quarter, "y", 2)
    piece = call(hidden_kernel, fast((PEERS * HID, LANES), BF16), (summands,))
    hidden = swapped(piece, TP, 4)
    results, shared_out, weight = call(
        down_kernel,
        (fast((ROWS, LANES), BF16), fast((16, LANES), F32), fast((16, ROWS), F32)),
        (hidden, expert_down, shared_down, routes, gates),
    )
    returned = swapped(results, "ep", 4)
    combined, squares = call(
        combine_kernel,
        (fast((16, LANES), F32), fast((PEERS, 1, LANES), F32)),
        (returned, weight, shared_out),
    )
    squares = swapped(squares, TP, 1)
    return call(
        final_kernel,
        jax.ShapeDtypeStruct((16, LANES), BF16),
        (squares, combined, out_gain),
    )


def solution(mesh):
    mesh = Mesh(mesh.devices.reshape(-1, 8, 4), ("ep", "y", "x"))
    in_specs = (
        P("ep", TP),
        P("ep", None),
        P("ep", None),
        P(TP),
        P("ep", TP, None),
        P("ep", TP, None),
        P("ep", None, TP),
        P(TP, None),
        P(TP, None),
        P(None, TP),
        P(TP),
    )
    return jax.shard_map(
        on_device, mesh=mesh, in_specs=in_specs, out_specs=P("ep", TP), check_vma=False
    )
```
